32 devices in a mesh: kv: 8 (over z, y), tp: 4 (over x, core).
Axes of the slice: x: 2, y: 2, z: 4, core: 2. Of those that a mesh axis runs over, the one named last changes fastest.
Arguments:
- tokens: bfloat16 [16, 4096], P(None, ('kv', 'tp')), may hold values from -8 to 8
- gate_weights: bfloat16 [2, 4096, 11264], P(None, None, ('kv', 'tp')), may hold values from -0.09375 to 0.09375
- up_weights: bfloat16 [2, 4096, 11264], P(None, None, ('kv', 'tp')), may hold values from -0.09375 to 0.09375
- down_weights: bfloat16 [2, 11264, 4096], P(None, ('kv', 'tp')), may hold values from -0.4375 to 0.4375
- norm_gain: bfloat16 [3, 4096], P(None, ('kv', 'tp')), may hold values from 0.25 to 4.5
- norm_bias: bfloat16 [3, 4096], P(None, ('kv', 'tp')), may hold values from -3 to 3
- query_weight: bfloat16 [4096, 4096], P('kv', 'tp'), may hold values from -0.09375 to 0.09375
- forget_weight: bfloat16 [4096, 4096], P('kv', 'tp'), may hold values from -0.09375 to 0.09375
- input_weight: bfloat16 [4096, 4096], P('kv', 'tp'), may hold values from -0.09375 to 0.09375
- outgate_weight: bfloat16 [4096, 4096], P('kv', 'tp'), may hold values from -0.09375 to 0.09375
- lower_bound: float32 [4096], P('tp'), may hold values from 0.05 to 0.9
- head_gain: float32 [4096], P('tp'), may hold values from 0.1 to 1.9
- out_weight: bfloat16 [4096, 4096], P('tp'), may hold values from -0.25 to 0.25
- state: float32 [16, 32, 128, 128], P('kv', 'tp'), may hold values from -3 to 3
Outputs:
- mixed: bfloat16 [16, 4096], P(None, ('kv', 'tp'))
- new_state: float32 [16, 32, 128, 128], P('kv', 'tp')
The draws below stay inside these ranges and needn't reach their ends.
All inputs are finite; a program needn't handle non-finite values.
Results may differ from the reference program's by a relative error of at most 0.022.
Values may be sent and summed in bfloat16 or wider, within the bound.
A program may use at most 64 MiB of HBM per device.

```python
import math
import jax
import jax.numpy as jnp
from jax import lax

D = 4096
FF = 11264
HEAD = 128
HEADS = 32
BATCH = 16


def draw_tokens(key, part):
    position = jnp.arange(D, dtype=jnp.float32)[None, :] / D
    values = jax.random.normal(key, (BATCH, D), jnp.float32) * 0.4 * 4.0 ** position
    return jnp.clip(values, -8.0, 8.0).astype(jnp.bfloat16)


def draw_norm_gain(key, part):
    position = jnp.arange(D, dtype=jnp.float32)[None, :] / D
    jitter = 1.0 + 0.3 * jax.random.uniform(key, (3, D), jnp.float32, -1.0, 1.0)
    values = 0.6 * 3.0 ** position * jitter
    return values.astype(jnp.bfloat16)


def with_spikes(result, own_key, source, target, parts, factor):
    owner, partner = [(jnp.arange(result.shape[dim]) // (result.shape[dim] // parts)).reshape([-1 if axis == dim else 1 for axis in range(result.ndim)]) for dim in (source, target)]
    chosen = jax.random.permutation(own_key, parts)[partner]
    strong = (owner == chosen) | (owner == (partner + parts // 2) % parts)
    return jnp.where(strong, factor * result, result)


def block_scale(key, dims, cuts, least, top_value):
    factor_of, own = 1.0, jax.random.fold_in(key, 6)
    for dim, blocks in cuts:
        steps = jnp.exp(jax.random.uniform(jax.random.fold_in(own, dim), (blocks,), jnp.float32, least / len(cuts), top_value / len(cuts)))
        factor_of = factor_of * jnp.repeat(steps, dims[dim] // blocks).reshape([-1 if axis == dim else 1 for axis in range(len(dims))])
    return factor_of


def noise(rng, shape, scale, bound, cuts=(), held_as=jnp.bfloat16):
    drawn = scale * jax.random.normal(rng, shape, jnp.float32)
    if cuts:
        drawn = drawn * block_scale(rng, shape, cuts, -0.22, 0.18)
    return jnp.clip(drawn, -bound, bound).astype(held_as)


def noise_with(rng, shape, scale, reach, cuts, heavy, held_as=jnp.bfloat16):
    array = scale * jax.random.normal(rng, shape, jnp.float32)
    if cuts:
        array = array * block_scale(rng, shape, cuts, -0.22, 0.18)
    return jnp.clip(with_spikes(array, jax.random.fold_in(rng, 3), *heavy), -reach, reach).astype(held_as)


def setup_inputs(seed: int = 0) -> dict:
    arg_keys = jax.random.split(jax.random.key(seed), 15)
    tokens = draw_tokens(jax.random.fold_in(arg_keys[14], 71), 0)
    gate_weights = noise(arg_keys[1], (2, D, FF), D ** -0.5, 0.09375, ((2, 32),))
    up_weights = noise(arg_keys[2], (2, D, FF), D ** -0.5, 0.09375, ((2, 32),))
    down_weights = noise_with(arg_keys[3], (2, FF, D), (FF // 16) ** -0.5, 0.4375, ((1, 32),), (1, 2, 32, 2.75))
    norm_gain = draw_norm_gain(jax.random.fold_in(arg_keys[14], 71), 0)
    norm_bias = noise(arg_keys[5], (3, D), 0.5, 3.0, ((1, 32),))
    query_weight = noise(arg_keys[6], (D, D), D ** -0.5, 0.09375, ((0, 8), (1, 4)))
    forget_weight = noise(arg_keys[7], (D, D), D ** -0.5, 0.09375, ((0, 8), (1, 4)))
    input_weight = noise(arg_keys[8], (D, D), D ** -0.5, 0.09375, ((0, 8), (1, 4)))
    outgate_weight = noise(arg_keys[9], (D, D), D ** -0.5, 0.09375, ((0, 8), (1, 4)))
    lower_bound = jnp.clip(jnp.exp(math.log(0.9) - 2.8903717 * jax.random.uniform(arg_keys[10], (D,), jnp.float32) ** block_scale(arg_keys[10], (D,), ((0, 4),), -0.2, 0.2)), 0.05, 0.9)
    head_gain = jnp.clip(1.0 + 0.18 * jax.random.normal(arg_keys[11], (D,), jnp.float32), 0.1, 1.9)
    out_weight = noise_with(arg_keys[12], (D, D), (D // 4) ** -0.5, 0.25, ((0, 4),), (0, 1, 4, 2.0))
    state = noise(arg_keys[13], (BATCH, HEADS, HEAD, HEAD), 0.5, 3.0, ((0, 8), (1, 4)), jnp.float32)
    return {"tokens": tokens, "gate_weights": gate_weights, "up_weights": up_weights, "down_weights": down_weights, "norm_gain": norm_gain, "norm_bias": norm_bias, "query_weight": query_weight, "forget_weight": forget_weight, "input_weight": input_weight, "outgate_weight": outgate_weight, "lower_bound": lower_bound, "head_gain": head_gain, "out_weight": out_weight, "state": state}


residual_scale = 8.0 ** 0.25
norm_eps = 1e-05
head_eps = 1e-06

def layer_norm(stream, gain_row, bias_row):
    row_mean = lax.optimization_barrier(jnp.mean(stream, axis=-1, keepdims=True))
    centred = stream - row_mean
    spread = lax.optimization_barrier(jnp.mean(centred * centred, axis=-1, keepdims=True))
    return centred * lax.rsqrt(spread + norm_eps) * gain_row.astype(jnp.float32) + bias_row.astype(jnp.float32)

def half_ffn(row_block, gate_w, up_w, down_w):
    gate_proj = jnp.dot(row_block, gate_w, preferred_element_type=jnp.float32)
    up_proj = jnp.dot(row_block, up_w, preferred_element_type=jnp.float32)
    hidden = (jax.nn.silu(gate_proj) * up_proj).astype(jnp.bfloat16)
    return jnp.dot(hidden, down_w, preferred_element_type=jnp.float32)

def reference(tokens, gate_weights, up_weights, down_weights, norm_gain, norm_bias, query_weight, forget_weight, input_weight, outgate_weight, lower_bound, head_gain, out_weight, state):
    head_count = D // HEAD
    row_count = tokens.shape[0]
    branch_one = half_ffn(tokens, gate_weights[0], up_weights[0], down_weights[0])
    stream = residual_scale * tokens.astype(jnp.float32) + 0.5 * branch_one
    normed = layer_norm(stream, norm_gain[0], norm_bias[0]).astype(jnp.bfloat16)
    projected = [jnp.dot(normed, weight, preferred_element_type=jnp.float32).astype(jnp.bfloat16) for weight in (query_weight, forget_weight, input_weight, outgate_weight)]
    shaped = [piece_pre.astype(jnp.float32).reshape(row_count, head_count, HEAD) for piece_pre in projected[:3]]
    low_bound = lower_bound.reshape(head_count, HEAD)

    def one_sequence(pieces):
        query_pre, forget_pre, input_pre, old_state = pieces
        forget = low_bound + (1.0 - low_bound) * jax.nn.sigmoid(forget_pre)
        key_part = (1.0 - low_bound) * jax.nn.sigmoid(-forget_pre)
        updated = forget[:, :, None] * old_state + key_part[:, :, None] * input_pre[:, None, :]
        readout = jnp.einsum('hd,hde->he', jax.nn.silu(query_pre), updated, precision=lax.Precision.HIGHEST)
        return (readout, updated)
    readout, new_state = lax.map(one_sequence, (shaped[0], shaped[1], shaped[2], state))
    readout = readout * lax.rsqrt(lax.optimization_barrier(jnp.mean(readout * readout, axis=-1, keepdims=True)) + head_eps)
    gated_out = (readout.reshape(row_count, D) * head_gain * jax.nn.silu(projected[3].astype(jnp.float32))).astype(jnp.bfloat16)
    mixed_out = jnp.dot(gated_out, out_weight, preferred_element_type=jnp.float32)
    stream = (residual_scale * normed.astype(jnp.float32) + mixed_out).astype(jnp.bfloat16)
    normed = layer_norm(stream.astype(jnp.float32), norm_gain[1], norm_bias[1]).astype(jnp.bfloat16)
    branch_two = half_ffn(normed, gate_weights[1], up_weights[1], down_weights[1])
    stream = residual_scale * normed.astype(jnp.float32) + 0.5 * branch_two
    mixed = layer_norm(stream, norm_gain[2], norm_bias[2]).astype(jnp.bfloat16)
    return (mixed, new_state)
```

```python
import functools

import jax
import jax.numpy as jnp
from jax import lax
from jax.experimental import pallas as pl
from jax.experimental.pallas import tpu as pltpu
from jax.sharding import PartitionSpec as P

MESH = pl.DeviceIdType.MESH

HEAD = 128


residual_scale = 8.0**0.25
norm_eps = 1e-05
head_eps = 1e-06


def whole_norm(stream, gain_row, bias_row):
    row_mean = jnp.mean(stream, axis=-1, keepdims=True)
    centred = stream - row_mean
    spread = jnp.mean(centred * centred, axis=-1, keepdims=True)
    return centred * lax.rsqrt(spread + norm_eps) * gain_row.astype(jnp.float32) + bias_row.astype(
        jnp.float32
    )


def ffn_partial(whole_rows, gate_w, up_w, down_w):
    gate_proj = jnp.dot(whole_rows, gate_w, preferred_element_type=jnp.float32)
    up_proj = jnp.dot(whole_rows, up_w, preferred_element_type=jnp.float32)
    hidden = (jax.nn.silu(gate_proj) * up_proj).astype(jnp.bfloat16)
    return jnp.dot(hidden, down_w, preferred_element_type=jnp.float32)


def local(
    tokens,
    gate_weights,
    up_weights,
    down_weights,
    norm_gain,
    norm_bias,
    query_weight,
    forget_weight,
    input_weight,
    outgate_weight,
    lower_bound,
    head_gain,
    out_weight,
    state,
):
    own_cols = tokens.shape[1]
    col_offset = lax.axis_index(("kv", "tp")) * own_cols
    whole_tokens, whole_gain, whole_bias = (
        lax.all_gather(tokens, ("kv", "tp"), axis=1, tiled=True),
        lax.all_gather(norm_gain, ("kv", "tp"), axis=1, tiled=True),
        lax.all_gather(norm_bias, ("kv", "tp"), axis=1, tiled=True),
    )

    def finish(partial_value, residual_whole, index, want_whole):
        total = lax.psum(partial_value, ("kv", "tp"))
        stream = residual_scale * residual_whole + 0.5 * total
        normed = whole_norm(stream, whole_gain[index], whole_bias[index]).astype(jnp.bfloat16)
        if want_whole:
            return normed
        return lax.dynamic_slice_in_dim(normed, col_offset, own_cols, 1)

    partial_one = ffn_partial(whole_tokens, gate_weights[0], up_weights[0], down_weights[0])
    normed_one = finish(partial_one, whole_tokens.astype(jnp.float32), 0, True)
    seq_count = state.shape[0]
    head_count = state.shape[1]
    head_cols = query_weight.shape[1]
    weight_rows = query_weight.shape[0]
    seq_offset = lax.axis_index("kv") * seq_count
    block_rows = lax.dynamic_slice_in_dim(
        normed_one, lax.axis_index("kv") * weight_rows, weight_rows, 1
    )
    weights = (query_weight, forget_weight, input_weight, outgate_weight)
    projected = lax.psum_scatter(
        jnp.concatenate(
            [jnp.dot(block_rows, weight, preferred_element_type=jnp.float32) for weight in weights],
            axis=1,
        ).astype(jnp.bfloat16),
        "kv",
        scatter_dimension=0,
        tiled=True,
    )
    query_pre = projected[:, :head_cols].astype(jnp.float32).reshape(seq_count, head_count, HEAD)
    forget_pre = (
        projected[:, head_cols : 2 * head_cols]
        .astype(jnp.float32)
        .reshape(seq_count, head_count, HEAD)
    )
    input_pre = (
        projected[:, 2 * head_cols : 3 * head_cols]
        .astype(jnp.float32)
        .reshape(seq_count, head_count, HEAD)
    )
    outgate_pre = projected[:, 3 * head_cols :].astype(jnp.float32)
    low_bound = lower_bound.reshape(head_count, HEAD)
    forget = low_bound + (1.0 - low_bound) * jax.nn.sigmoid(forget_pre)
    key_part = (1.0 - low_bound) * jax.nn.sigmoid(-forget_pre)
    updated = forget[..., None] * state + key_part[..., None] * input_pre[:, :, None, :]
    readout = jnp.einsum(
        "shd,shde->she", jax.nn.silu(query_pre), updated, precision=lax.Precision.HIGHEST
    )
    readout = readout * lax.rsqrt(jnp.mean(readout * readout, axis=-1, keepdims=True) + head_eps)
    gated_out = (
        readout.reshape(seq_count, head_cols) * head_gain * jax.nn.silu(outgate_pre)
    ).astype(jnp.bfloat16)
    mixer_part = jnp.dot(gated_out, out_weight, preferred_element_type=jnp.float32)
    head_sum = lax.psum_scatter(
        mixer_part.astype(jnp.bfloat16), "tp", scatter_dimension=1, tiled=True
    ).astype(jnp.float32)
    piece_cols = head_sum.shape[1]
    own_normed = lax.dynamic_slice_in_dim(normed_one, seq_offset, seq_count, 0)
    own_normed = lax.dynamic_slice_in_dim(
        own_normed, lax.axis_index("tp") * piece_cols, piece_cols, 1
    )
    stream_own = (residual_scale * own_normed.astype(jnp.float32) + head_sum).astype(jnp.bfloat16)
    seq_rows = lax.all_gather(stream_own, "tp", axis=1, tiled=True)
    stream_two = lax.all_gather(seq_rows, "kv", axis=0, tiled=True)
    normed_two = whole_norm(stream_two.astype(jnp.float32), whole_gain[1], whole_bias[1]).astype(
        jnp.bfloat16
    )
    partial_two = ffn_partial(normed_two, gate_weights[1], up_weights[1], down_weights[1])
    mixed = finish(partial_two, normed_two.astype(jnp.float32), 2, False)
    return (mixed, updated)


TOK, GB, RS_ONE, AG_ONE, RS_KV, RS_TP, AG_TWO, RS_THREE, AG_THREE = range(9)
PHASES = 9


def tree_sum(terms):
    while len(terms) > 1:
        rest = [terms[-1]] if len(terms) % 2 else []
        terms = [a + b for a, b in zip(terms[::2], terms[1::2])] + rest
    return terms[0]


def layer_kernel(
    n_kv,
    n_tp,
    tokens_ref,
    gain_ref,
    bias_ref,
    low_ref,
    head_gain_ref,
    gate_hbm,
    up_hbm,
    down_hbm,
    query_hbm,
    forget_hbm,
    input_hbm,
    outgate_hbm,
    out_hbm,
    state_hbm,
    mixed_ref,
    state_out,
    gate_v,
    up_v,
    down_v,
    proj_v,
    out_v,
    state_v,
    new_v,
    tok_buf,
    gb_own,
    gb_buf,
    rs_send,
    rs_recv_one,
    rs_recv_three,
    own_ag,
    ag_one,
    normed_f32,
    normed_bf,
    proj_f32,
    proj_send,
    proj_recv,
    gated_buf,
    tp_f32,
    tp_send,
    tp_recv,
    own_ag_two,
    ag_two,
    ag_two_f32,
    own_ag_three,
    ag_three,
    final_buf,
    send_sem,
    recv_sem,
    load_sem,
    store_sem,
):
    n = n_kv * n_tp
    batch, lane = tokens_ref.shape
    width = n * lane
    seqs, heads = state_v.shape[0], state_v.shape[1]
    kv, tp = lax.axis_index("kv"), lax.axis_index("tp")
    me = kv * n_tp + tp

    proj_hbm = (query_hbm, forget_hbm, input_hbm, outgate_hbm)
    loads = {}
    order = [("gate0", gate_hbm.at[0], gate_v.at[0]), ("up0", up_hbm.at[0], up_v.at[0])]
    order += [("down0", down_hbm.at[0], down_v.at[0])]
    order += [("proj%d" % i, proj_hbm[i], proj_v.at[i]) for i in range(4)]
    order += [("state", state_hbm, state_v), ("out", out_hbm, out_v)]
    order += [("gate1", gate_hbm.at[1], gate_v.at[1]), ("up1", up_hbm.at[1], up_v.at[1])]
    order += [("down1", down_hbm.at[1], down_v.at[1])]
    for i, (name, source, target) in enumerate(order):
        loads[name] = pltpu.make_async_copy(source, target, load_sem.at[i])
        loads[name].start()

    def peer_id(k):
        peer = lax.rem(me + k, n)
        return peer, (lax.div(peer, n_tp), lax.rem(peer, n_tp))

    barrier = pltpu.get_barrier_semaphore()

    @pl.loop(1, n)
    def _(k):
        _, device = peer_id(k)
        pl.semaphore_signal(barrier, inc=1, device_id=device, device_id_type=MESH)

    def slot(ref, index, rows):
        return ref.at[pl.ds(pl.multiple_of(index * rows, rows), rows)]

    def send_all(phase, src_of, dst, count, device_of):
        @pl.loop(1, count)
        def _(k):
            index, device = device_of(k)
            pltpu.make_async_remote_copy(
                src_ref=src_of(index),
                dst_ref=dst,
                send_sem=send_sem.at[phase],
                recv_sem=recv_sem.at[phase],
                device_id=device,
                device_id_type=MESH,
            ).start()

    def wait_bytes(sem, ref, rows):
        part = ref.at[pl.ds(0, rows)]
        pltpu.make_async_copy(part, part, sem).wait()

    gb_own[...] = jnp.zeros(gb_own.shape, jnp.float32)
    gb_own[0:3, :] = gain_ref[...].astype(jnp.float32)
    gb_own[3:6, :] = bias_ref[...].astype(jnp.float32)
    slot(gb_buf, me, 8)[...] = gb_own[...]
    slot(tok_buf, me, batch)[...] = tokens_ref[...]

    pl.semaphore_wait(barrier, n - 1)
    send_all(TOK, lambda i: tokens_ref, slot(tok_buf, me, batch), n, peer_id)
    send_all(GB, lambda i: gb_own, slot(gb_buf, me, 8), n, peer_id)

    def tiles_of(ref):
        return [ref[j * batch : (j + 1) * batch, :].astype(jnp.float32) for j in range(n)]

    def stats(tiles):
        mean = jnp.sum(tree_sum(tiles), axis=1, keepdims=True) / width
        centred = [tile - mean for tile in tiles]
        spread = jnp.sum(tree_sum([c * c for c in centred]), axis=1, keepdims=True) / width
        return mean, centred, lax.rsqrt(spread + norm_eps)

    def norm_tiles(tiles, index):
        _, centred, scale = stats(tiles)
        return [
            c * scale * gb_buf[8 * j + index : 8 * j + index + 1, :]
            + gb_buf[8 * j + 3 + index : 8 * j + 4 + index, :]
            for j, c in enumerate(centred)
        ]

    def ffn(rows, layer):
        step = 4 * lane
        gate = jnp.zeros((batch, gate_v.shape[2]), jnp.float32)
        up = jnp.zeros((batch, gate_v.shape[2]), jnp.float32)
        loads["gate%d" % layer].wait()
        loads["up%d" % layer].wait()
        for k in range(0, width, step):
            piece = rows[:, k : k + step]
            gate += jnp.dot(
                piece, gate_v[layer, k : k + step, :], preferred_element_type=jnp.float32
            )
            up += jnp.dot(piece, up_v[layer, k : k + step, :], preferred_element_type=jnp.float32)
        hidden = (jax.nn.silu(gate) * up).astype(jnp.bfloat16)
        loads["down%d" % layer].wait()
        for k in range(0, width, step):
            part = jnp.dot(
                hidden, down_v[layer, :, k : k + step], preferred_element_type=jnp.float32
            ).astype(jnp.bfloat16)
            for j in range(step // lane):
                first = (k // lane + j) * batch
                rs_send[first : first + batch, :] = part[:, j * lane : (j + 1) * lane]

    def reduce_scatter(phase, recv):
        send_all(phase, lambda i: slot(rs_send, i, batch), slot(recv, me, batch), n, peer_id)
        slot(recv, me, batch)[...] = slot(rs_send, me, batch)[...]
        wait_bytes(recv_sem.at[phase], recv, (n - 1) * batch)
        return tree_sum(tiles_of(recv))

    wait_bytes(recv_sem.at[TOK], tok_buf, (n - 1) * batch)
    ffn(jnp.concatenate([tok_buf[j * batch : (j + 1) * batch, :] for j in range(n)], axis=1), 0)
    total = reduce_scatter(RS_ONE, rs_recv_one)
    stream = residual_scale * tokens_ref[...].astype(jnp.float32) + 0.5 * total
    own_ag[...] = stream.astype(jnp.bfloat16)
    slot(ag_one, me, batch)[...] = stream.astype(jnp.bfloat16)
    send_all(AG_ONE, lambda i: own_ag, slot(ag_one, me, batch), n, peer_id)
    wait_bytes(recv_sem.at[GB], gb_buf, (n - 1) * 8)
    wait_bytes(recv_sem.at[AG_ONE], ag_one, (n - 1) * batch)
    for j, tile in enumerate(norm_tiles(tiles_of(ag_one), 0)):
        rounded = tile.astype(jnp.bfloat16)
        normed_bf[j * batch : (j + 1) * batch, :] = rounded
        normed_f32[j * batch : (j + 1) * batch, :] = rounded.astype(jnp.float32)

    own_rows = slot(normed_bf, kv, n_tp * batch)
    block = jnp.concatenate(
        [own_rows[j * batch : (j + 1) * batch, :] for j in range(n_tp)], axis=1
    )
    per_seq = 4 * heads
    for i in range(4):
        loads["proj%d" % i].wait()
        part = jnp.dot(block, proj_v[i], preferred_element_type=jnp.float32)
        for h in range(heads):
            for r in range(0, batch, 8):
                proj_f32[pl.ds(r * per_seq + i * heads + h, 8, stride=per_seq), :] = part[
                    r : r + 8, h * HEAD : (h + 1) * HEAD
                ]
    proj_send[...] = proj_f32[...].astype(jnp.bfloat16)
    block_len = seqs * per_seq

    def kv_peer(k):
        peer = lax.rem(kv + k, n_kv)
        return peer, (peer, tp)

    send_all(
        RS_KV,
        lambda i: slot(proj_send, i, block_len),
        slot(proj_recv, kv, block_len),
        n_kv,
        kv_peer,
    )
    slot(proj_recv, kv, block_len)[...] = slot(proj_send, kv, block_len)[...]
    wait_bytes(recv_sem.at[RS_KV], proj_recv, (n_kv - 1) * block_len)
    projected = tree_sum(
        [
            proj_recv[j * block_len : (j + 1) * block_len, :].astype(jnp.float32)
            for j in range(n_kv)
        ]
    )
    projected = projected.astype(jnp.bfloat16).astype(jnp.float32)

    low = low_ref[...]
    loads["state"].wait()
    for s in range(seqs):
        base = s * per_seq
        query_pre = projected[base : base + heads]
        forget_pre = projected[base + heads : base + 2 * heads]
        input_pre = projected[base + 2 * heads : base + 3 * heads]
        outgate_pre = projected[base + 3 * heads : base + 4 * heads]
        forget = low + (1.0 - low) * jax.nn.sigmoid(forget_pre)
        key_part = (1.0 - low) * jax.nn.sigmoid(-forget_pre)
        fill = jnp.zeros((HEAD - 3 * heads, HEAD), jnp.float32)
        turned = jnp.concatenate([forget, key_part, jax.nn.silu(query_pre), fill], axis=0).T
        readouts = []
        for h in range(heads):
            updated = (
                turned[:, h : h + 1] * state_v[s, h]
                + turned[:, heads + h : heads + h + 1] * input_pre[h : h + 1, :]
            )
            new_v[s, h] = updated
            query_col = turned[:, 2 * heads + h : 2 * heads + h + 1]
            readouts.append(jnp.sum(query_col * updated, axis=0, keepdims=True))
        readout = jnp.concatenate(readouts, axis=0)
        mean_square = jnp.mean(readout * readout, axis=1, keepdims=True)
        readout = readout * lax.rsqrt(mean_square + head_eps)
        gated_buf[s * heads : (s + 1) * heads, :] = (
            readout * head_gain_ref[...] * jax.nn.silu(outgate_pre)
        )
    store = pltpu.make_async_copy(new_v, state_out, store_sem)
    store.start()

    gated = jnp.concatenate(
        [gated_buf[pl.ds(h, seqs, stride=heads), :] for h in range(heads)], axis=1
    ).astype(jnp.bfloat16)
    loads["out"].wait()
    step = 4 * lane
    rows_tp = seqs * heads
    for k in range(0, width, step):
        part = jnp.dot(gated, out_v[:, k : k + step], preferred_element_type=jnp.float32)
        for j in range(step // lane):
            tile = k // lane + j
            first = (tile // heads) * rows_tp + tile % heads
            tp_f32[pl.ds(first, seqs, stride=heads), :] = part[:, j * lane : (j + 1) * lane]
    tp_send[...] = tp_f32[...].astype(jnp.bfloat16)

    def tp_peer(k):
        peer = lax.rem(tp + k, n_tp)
        return peer, (kv, peer)

    send_all(
        RS_TP, lambda i: slot(tp_send, i, rows_tp), slot(tp_recv, tp, rows_tp), n_tp, tp_peer
    )
    slot(tp_recv, tp, rows_tp)[...] = slot(tp_send, tp, rows_tp)[...]
    residual = jnp.concatenate(
        [
            normed_f32[pl.ds(tp * (heads * batch) + kv * seqs + s, heads, stride=batch), :]
            for s in range(seqs)
        ],
        axis=0,
    )
    wait_bytes(recv_sem.at[RS_TP], tp_recv, (n_tp - 1) * rows_tp)
    head_sum = tree_sum(
        [tp_recv[j * rows_tp : (j + 1) * rows_tp, :].astype(jnp.float32) for j in range(n_tp)]
    )
    stream_two = (residual_scale * residual + head_sum).astype(jnp.bfloat16)
    own_ag_two[...] = stream_two
    slot(ag_two, me, rows_tp)[...] = stream_two
    send_all(AG_TWO, lambda i: own_ag_two, slot(ag_two, me, rows_tp), n, peer_id)
    wait_bytes(recv_sem.at[AG_TWO], ag_two, (n - 1) * rows_tp)
    ag_two_f32[...] = ag_two[...].astype(jnp.float32)
    tiles = [
        jnp.concatenate(
            [
                ag_two_f32[
                    pl.ds((j // heads) * rows_tp + s * heads + j % heads, n_kv, stride=n_tp * rows_tp),
                    :,
                ]
                for s in range(seqs)
            ],
            axis=0,
        )
        for j in range(n)
    ]
    normed = [tile.astype(jnp.bfloat16) for tile in norm_tiles(tiles, 1)]
    wait_bytes(send_sem.at[RS_ONE], rs_recv_one, (n - 1) * batch)
    for j, tile in enumerate(normed):
        normed_bf[j * batch : (j + 1) * batch, :] = tile
    ffn(jnp.concatenate(normed, axis=1), 1)
    total = reduce_scatter(RS_THREE, rs_recv_three)
    residual = slot(normed_bf, me, batch)[...].astype(jnp.float32)
    stream = residual_scale * residual + 0.5 * total
    own_ag_three[...] = stream.astype(jnp.bfloat16)
    slot(ag_three, me, batch)[...] = stream.astype(jnp.bfloat16)
    send_all(AG_THREE, lambda i: own_ag_three, slot(ag_three, me, batch), n, peer_id)
    wait_bytes(recv_sem.at[AG_THREE], ag_three, (n - 1) * batch)
    mean, _, scale = stats(tiles_of(ag_three))
    mixed = (stream - mean) * scale * gb_own[2:3, :] + gb_own[5:6, :]
    for s in range(seqs):
        final_buf[pl.ds(s, n_kv, stride=seqs), :] = mixed[s * n_kv : (s + 1) * n_kv, :]
    mixed_ref[...] = final_buf[...].astype(jnp.bfloat16)

    for phase in (TOK, AG_ONE, AG_TWO, RS_THREE, AG_THREE):
        wait_bytes(send_sem.at[phase], tok_buf, (n - 1) * batch)
    wait_bytes(send_sem.at[GB], gb_buf, (n - 1) * 8)
    wait_bytes(send_sem.at[RS_KV], proj_recv, (n_kv - 1) * block_len)
    wait_bytes(send_sem.at[RS_TP], tp_recv, (n_tp - 1) * rows_tp)
    store.wait()


def fused(n_kv, n_tp, *args):
    (
        tokens,
        gate_weights,
        up_weights,
        down_weights,
        norm_gain,
        norm_bias,
        query_weight,
        forget_weight,
        input_weight,
        outgate_weight,
        lower_bound,
        head_gain,
        out_weight,
        state,
    ) = args
    batch, lane = tokens.shape
    n = n_kv * n_tp
    seqs, heads = state.shape[:2]
    bf16, f32 = jnp.bfloat16, jnp.float32
    per_seq = 4 * heads
    rows_tp = seqs * heads
    scratch = [
        pltpu.VMEM(gate_weights.shape, bf16),
        pltpu.VMEM(up_weights.shape, bf16),
        pltpu.VMEM(down_weights.shape, bf16),
        pltpu.VMEM((4, *query_weight.shape), bf16),
        pltpu.VMEM(out_weight.shape, bf16),
        pltpu.VMEM(state.shape, f32),
        pltpu.VMEM(state.shape, f32),
        pltpu.VMEM((n * batch, lane), bf16),
        pltpu.VMEM((8, lane), f32),
        pltpu.VMEM((n * 8, lane), f32),
        pltpu.VMEM((n * batch, lane), bf16),
        pltpu.VMEM((n * batch, lane), bf16),
        pltpu.VMEM((n * batch, lane), bf16),
        pltpu.VMEM((batch, lane), bf16),
        pltpu.VMEM((n * batch, lane), bf16),
        pltpu.VMEM((n * batch, lane), f32),
        pltpu.VMEM((n * batch, lane), bf16),
        pltpu.VMEM((batch * per_seq, HEAD), f32),
        pltpu.VMEM((batch * per_seq, HEAD), bf16),
        pltpu.VMEM((batch * per_seq, HEAD), bf16),
        pltpu.VMEM((rows_tp, HEAD), f32),
        pltpu.VMEM((n_tp * rows_tp, HEAD), f32),
        pltpu.VMEM((n_tp * rows_tp, HEAD), bf16),
        pltpu.VMEM((n_tp * rows_tp, HEAD), bf16),
        pltpu.VMEM((rows_tp, HEAD), bf16),
        pltpu.VMEM((n * rows_tp, HEAD), bf16),
        pltpu.VMEM((n * rows_tp, HEAD), f32),
        pltpu.VMEM((batch, lane), bf16),
        pltpu.VMEM((n * batch, lane), bf16),
        pltpu.VMEM((batch, lane), f32),
        pltpu.SemaphoreType.DMA((PHASES,)),
        pltpu.SemaphoreType.DMA((PHASES,)),
        pltpu.SemaphoreType.DMA((12,)),
        pltpu.SemaphoreType.DMA,
    ]
    vmem = pl.BlockSpec(memory_space=pltpu.VMEM)
    hbm = pl.BlockSpec(memory_space=pl.ANY)
    return pl.pallas_call(
        functools.partial(layer_kernel, n_kv, n_tp),
        out_shape=(
            jax.ShapeDtypeStruct(tokens.shape, bf16),
            jax.ShapeDtypeStruct(state.shape, f32),
        ),
        in_specs=[vmem] * 5 + [hbm] * 9,
        out_specs=(vmem, hbm),
        scratch_shapes=scratch,
        compiler_params=pltpu.CompilerParams(
            collective_id=0, has_side_effects=True, vmem_limit_bytes=60 * 1024 * 1024
        ),
        name="layer",
    )(
        tokens,
        norm_gain,
        norm_bias,
        lower_bound.reshape(heads, HEAD),
        head_gain.reshape(heads, HEAD),
        gate_weights,
        up_weights,
        down_weights,
        query_weight,
        forget_weight,
        input_weight,
        outgate_weight,
        out_weight,
        state,
    )


def dispatch(n_kv, n_tp, *args):
    tokens, state = args[0], args[13]
    batch, lane = tokens.shape
    whole_tiles = lane == HEAD and batch % 16 == 0 and (state.shape[0] * state.shape[1]) % 16 == 0
    if whole_tiles and state.shape[1] == 8 and n_kv % 8 == 0:
        return fused(n_kv, n_tp, *args)
    return local(*args)


def solution(mesh):
    n_kv, n_tp = mesh.shape["kv"], mesh.shape["tp"]
    return jax.shard_map(
        functools.partial(dispatch, n_kv, n_tp),
        mesh=mesh,
        in_specs=(
            P(None, ("kv", "tp")),
            P(None, None, ("kv", "tp")),
            P(None, None, ("kv", "tp")),
            P(None, ("kv", "tp"), None),
            P(None, ("kv", "tp")),
            P(None, ("kv", "tp")),
            P("kv", "tp"),
            P("kv", "tp"),
            P("kv", "tp"),
            P("kv", "tp"),
            P("tp"),
            P("tp"),
            P("tp", None),
            P("kv", "tp", None, None),
        ),
        out_specs=(P(None, ("kv", "tp")), P("kv", "tp", None, None)),
        check_vma=False,
    )
```

```python
import functools

import jax
import jax.numpy as jnp
from jax import lax
from jax.experimental import pallas as pl
from jax.experimental.pallas import tpu as pltpu
from jax.sharding import PartitionSpec as P

MESH = pl.DeviceIdType.MESH

HEAD = 128


residual_scale = 8.0**0.25
norm_eps = 1e-05
head_eps = 1e-06


def whole_norm(stream, gain_row, bias_row):
    row_mean = jnp.mean(stream, axis=-1, keepdims=True)
    centred = stream - row_mean
    spread = jnp.mean(centred * centred, axis=-1, keepdims=True)
    return centred * lax.rsqrt(spread + norm_eps) * gain_row.astype(jnp.float32) + bias_row.astype(
        jnp.float32
    )


def ffn_partial(whole_rows, gate_w, up_w, down_w):
    gate_proj = jnp.dot(whole_rows, gate_w, preferred_element_type=jnp.float32)
    up_proj = jnp.dot(whole_rows, up_w, preferred_element_type=jnp.float32)
    hidden = (jax.nn.silu(gate_proj) * up_proj).astype(jnp.bfloat16)
    return jnp.dot(hidden, down_w, preferred_element_type=jnp.float32)


def local(
    tokens,
    gate_weights,
    up_weights,
    down_weights,
    norm_gain,
    norm_bias,
    query_weight,
    forget_weight,
    input_weight,
    outgate_weight,
    lower_bound,
    head_gain,
    out_weight,
    state,
):
    own_cols = tokens.shape[1]
    col_offset = lax.axis_index(("kv", "tp")) * own_cols
    whole_tokens, whole_gain, whole_bias = (
        lax.all_gather(tokens, ("kv", "tp"), axis=1, tiled=True),
        lax.all_gather(norm_gain, ("kv", "tp"), axis=1, tiled=True),
        lax.all_gather(norm_bias, ("kv", "tp"), axis=1, tiled=True),
    )

    def finish(partial_value, residual_whole, index, want_whole):
        total = lax.psum(partial_value, ("kv", "tp"))
        stream = residual_scale * residual_whole + 0.5 * total
        normed = whole_norm(stream, whole_gain[index], whole_bias[index]).astype(jnp.bfloat16)
        if want_whole:
            return normed
        return lax.dynamic_slice_in_dim(normed, col_offset, own_cols, 1)

    partial_one = ffn_partial(whole_tokens, gate_weights[0], up_weights[0], down_weights[0])
    normed_one = finish(partial_one, whole_tokens.astype(jnp.float32), 0, True)
    seq_count = state.shape[0]
    head_count = state.shape[1]
    head_cols = query_weight.shape[1]
    weight_rows = query_weight.shape[0]
    seq_offset = lax.axis_index("kv") * seq_count
    block_rows = lax.dynamic_slice_in_dim(
        normed_one, lax.axis_index("kv") * weight_rows, weight_rows, 1
    )
    weights = (query_weight, forget_weight, input_weight, outgate_weight)
    projected = lax.psum_scatter(
        jnp.concatenate(
            [jnp.dot(block_rows, weight, preferred_element_type=jnp.float32) for weight in weights],
            axis=1,
        ).astype(jnp.bfloat16),
        "kv",
        scatter_dimension=0,
        tiled=True,
    )
    query_pre = projected[:, :head_cols].astype(jnp.float32).reshape(seq_count, head_count, HEAD)
    forget_pre = (
        projected[:, head_cols : 2 * head_cols]
        .astype(jnp.float32)
        .reshape(seq_count, head_count, HEAD)
    )
    input_pre = (
        projected[:, 2 * head_cols : 3 * head_cols]
        .astype(jnp.float32)
        .reshape(seq_count, head_count, HEAD)
    )
    outgate_pre = projected[:, 3 * head_cols :].astype(jnp.float32)
    low_bound = lower_bound.reshape(head_count, HEAD)
    forget = low_bound + (1.0 - low_bound) * jax.nn.sigmoid(forget_pre)
    key_part = (1.0 - low_bound) * jax.nn.sigmoid(-forget_pre)
    updated = forget[..., None] * state + key_part[..., None] * input_pre[:, :, None, :]
    readout = jnp.einsum(
        "shd,shde->she", jax.nn.silu(query_pre), updated, precision=lax.Precision.HIGHEST
    )
    readout = readout * lax.rsqrt(jnp.mean(readout * readout, axis=-1, keepdims=True) + head_eps)
    gated_out = (
        readout.reshape(seq_count, head_cols) * head_gain * jax.nn.silu(outgate_pre)
    ).astype(jnp.bfloat16)
    mixer_part = jnp.dot(gated_out, out_weight, preferred_element_type=jnp.float32)
    head_sum = lax.psum_scatter(
        mixer_part.astype(jnp.bfloat16), "tp", scatter_dimension=1, tiled=True
    ).astype(jnp.float32)
    piece_cols = head_sum.shape[1]
    own_normed = lax.dynamic_slice_in_dim(normed_one, seq_offset, seq_count, 0)
    own_normed = lax.dynamic_slice_in_dim(
        own_normed, lax.axis_index("tp") * piece_cols, piece_cols, 1
    )
    stream_own = (residual_scale * own_normed.astype(jnp.float32) + head_sum).astype(jnp.bfloat16)
    seq_rows = lax.all_gather(stream_own, "tp", axis=1, tiled=True)
    stream_two = lax.all_gather(seq_rows, "kv", axis=0, tiled=True)
    normed_two = whole_norm(stream_two.astype(jnp.float32), whole_gain[1], whole_bias[1]).astype(
        jnp.bfloat16
    )
    partial_two = ffn_partial(normed_two, gate_weights[1], up_weights[1], down_weights[1])
    mixed = finish(partial_two, normed_two.astype(jnp.float32), 2, False)
    return (mixed, updated)


TOK, GB, RS_ONE, AG_ONE, RS_KV, RS_TP, AG_TWO, RS_THREE, AG_THREE = range(9)
PHASES = 9


def tree_sum(terms):
    while len(terms) > 1:
        rest = [terms[-1]] if len(terms) % 2 else []
        terms = [a + b for a, b in zip(terms[::2], terms[1::2])] + rest
    return terms[0]


def dot_turned(rows, weights):
    return lax.dot_general(
        rows, weights, (((1,), (1,)), ((), ())), preferred_element_type=jnp.float32
    )


def layer_kernel(
    n_kv,
    n_tp,
    tokens_ref,
    gain_ref,
    bias_ref,
    low_ref,
    head_gain_ref,
    gate_hbm,
    up_hbm,
    down_hbm,
    query_hbm,
    forget_hbm,
    input_hbm,
    outgate_hbm,
    out_hbm,
    state_hbm,
    mixed_ref,
    state_out,
    gate_v,
    up_v,
    down_v,
    proj_v,
    out_v,
    state_v,
    new_v,
    tok_buf,
    gb_own,
    gb_buf,
    rs_send,
    rs_recv_one,
    rs_recv_three,
    own_ag,
    ag_one,
    normed_f32,
    normed_bf,
    proj_f32,
    proj_send,
    proj_recv,
    gated_buf,
    tp_f32,
    tp_send,
    tp_recv,
    own_ag_two,
    ag_two,
    ag_two_f32,
    own_ag_three,
    ag_three,
    final_buf,
    send_sem,
    recv_sem,
    load_sem,
    store_sem,
):
    n = n_kv * n_tp
    batch, lane = tokens_ref.shape
    width = n * lane
    seqs, heads = state_v.shape[0], state_v.shape[1]
    kv, tp = lax.axis_index("kv"), lax.axis_index("tp")
    me = kv * n_tp + tp

    proj_hbm = (query_hbm, forget_hbm, input_hbm, outgate_hbm)
    loads = {}
    order = [("gate0", gate_hbm.at[0], gate_v.at[0]), ("up0", up_hbm.at[0], up_v.at[0])]
    order += [("down0", down_hbm.at[0], down_v.at[0])]
    order += [("proj%d" % i, proj_hbm[i], proj_v.at[i]) for i in range(4)]
    order += [("state", state_hbm, state_v), ("out", out_hbm, out_v)]
    order += [("gate1", gate_hbm.at[1], gate_v.at[1]), ("up1", up_hbm.at[1], up_v.at[1])]
    order += [("down1", down_hbm.at[1], down_v.at[1])]
    for i, (name, source, target) in enumerate(order):
        loads[name] = pltpu.make_async_copy(source, target, load_sem.at[i])
        loads[name].start()

    def peer_id(k):
        peer = lax.rem(me + k, n)
        return peer, (lax.div(peer, n_tp), lax.rem(peer, n_tp))

    barrier = pltpu.get_barrier_semaphore()

    @pl.loop(1, n)
    def _(k):
        _, device = peer_id(k)
        pl.semaphore_signal(barrier, inc=1, device_id=device, device_id_type=MESH)

    def slot(ref, index, rows):
        return ref.at[pl.ds(pl.multiple_of(index * rows, rows), rows)]

    def send_all(phase, src_of, dst, count, device_of):
        @pl.loop(1, count)
        def _(k):
            index, device = device_of(k)
            pltpu.make_async_remote_copy(
                src_ref=src_of(index),
                dst_ref=dst,
                send_sem=send_sem.at[phase],
                recv_sem=recv_sem.at[phase],
                device_id=device,
                device_id_type=MESH,
            ).start()

    def wait_bytes(sem, ref, rows):
        part = ref.at[pl.ds(0, rows)]
        pltpu.make_async_copy(part, part, sem).wait()

    gb_own[...] = jnp.zeros(gb_own.shape, jnp.float32)
    gb_own[0:3, :] = gain_ref[...].astype(jnp.float32)
    gb_own[3:6, :] = bias_ref[...].astype(jnp.float32)
    slot(gb_buf, me, 8)[...] = gb_own[...]
    slot(tok_buf, me, batch)[...] = tokens_ref[...]

    pl.semaphore_wait(barrier, n - 1)
    send_all(TOK, lambda i: tokens_ref, slot(tok_buf, me, batch), n, peer_id)
    send_all(GB, lambda i: gb_own, slot(gb_buf, me, 8), n, peer_id)

    def tiles_of(ref):
        return [ref[j * batch : (j + 1) * batch, :].astype(jnp.float32) for j in range(n)]

    def stats(tiles):
        mean = jnp.sum(tree_sum(tiles), axis=1, keepdims=True) / width
        centred = [tile - mean for tile in tiles]
        spread = jnp.sum(tree_sum([c * c for c in centred]), axis=1, keepdims=True) / width
        return mean, centred, lax.rsqrt(spread + norm_eps)

    def norm_tiles(tiles, index):
        _, centred, scale = stats(tiles)
        return [
            c * scale * gb_buf[8 * j + index : 8 * j + index + 1, :]
            + gb_buf[8 * j + 3 + index : 8 * j + 4 + index, :]
            for j, c in enumerate(centred)
        ]

    def ffn(rows, layer):
        step = 4 * lane
        gate = jnp.zeros((batch, gate_v.shape[1]), jnp.float32)
        up = jnp.zeros((batch, gate_v.shape[1]), jnp.float32)
        loads["gate%d" % layer].wait()
        loads["up%d" % layer].wait()
        for k in range(0, width, step):
            piece = rows[:, k : k + step]
            gate += dot_turned(piece, gate_v[layer, :, k : k + step])
            up += dot_turned(piece, up_v[layer, :, k : k + step])
        hidden = (jax.nn.silu(gate) * up).astype(jnp.bfloat16)
        loads["down%d" % layer].wait()
        for k in range(0, width, step):
            part = jnp.dot(
                hidden, down_v[layer, :, k : k + step], preferred_element_type=jnp.float32
            ).astype(jnp.bfloat16)
            for j in range(step // lane):
                first = (k // lane + j) * batch
                rs_send[first : first + batch, :] = part[:, j * lane : (j + 1) * lane]

    def reduce_scatter(phase, recv):
        send_all(phase, lambda i: slot(rs_send, i, batch), slot(recv, me, batch), n, peer_id)
        slot(recv, me, batch)[...] = slot(rs_send, me, batch)[...]
        wait_bytes(recv_sem.at[phase], recv, (n - 1) * batch)
        return tree_sum(tiles_of(recv))

    wait_bytes(recv_sem.at[TOK], tok_buf, (n - 1) * batch)
    ffn(jnp.concatenate([tok_buf[j * batch : (j + 1) * batch, :] for j in range(n)], axis=1), 0)
    total = reduce_scatter(RS_ONE, rs_recv_one)
    stream = residual_scale * tokens_ref[...].astype(jnp.float32) + 0.5 * total
    own_ag[...] = stream.astype(jnp.bfloat16)
    slot(ag_one, me, batch)[...] = stream.astype(jnp.bfloat16)
    send_all(AG_ONE, lambda i: own_ag, slot(ag_one, me, batch), n, peer_id)
    wait_bytes(recv_sem.at[GB], gb_buf, (n - 1) * 8)
    wait_bytes(recv_sem.at[AG_ONE], ag_one, (n - 1) * batch)
    for j, tile in enumerate(norm_tiles(tiles_of(ag_one), 0)):
        rounded = tile.astype(jnp.bfloat16)
        normed_bf[j * batch : (j + 1) * batch, :] = rounded
        normed_f32[j * batch : (j + 1) * batch, :] = rounded.astype(jnp.float32)

    own_rows = slot(normed_bf, kv, n_tp * batch)
    block = jnp.concatenate(
        [own_rows[j * batch : (j + 1) * batch, :] for j in range(n_tp)], axis=1
    )
    per_seq = 4 * heads
    for i in range(4):
        loads["proj%d" % i].wait()
        part = jnp.dot(block, proj_v[i], preferred_element_type=jnp.float32)
        for h in range(heads):
            for r in range(0, batch, 8):
                proj_f32[pl.ds(r * per_seq + i * heads + h, 8, stride=per_seq), :] = part[
                    r : r + 8, h * HEAD : (h + 1) * HEAD
                ]
    proj_send[...] = proj_f32[...].astype(jnp.bfloat16)
    block_len = seqs * per_seq

    def kv_peer(k):
        peer = lax.rem(kv + k, n_kv)
        return peer, (peer, tp)

    send_all(
        RS_KV,
        lambda i: slot(proj_send, i, block_len),
        slot(proj_recv, kv, block_len),
        n_kv,
        kv_peer,
    )
    slot(proj_recv, kv, block_len)[...] = slot(proj_send, kv, block_len)[...]
    wait_bytes(recv_sem.at[RS_KV], proj_recv, (n_kv - 1) * block_len)
    projected = tree_sum(
        [
            proj_recv[j * block_len : (j + 1) * block_len, :].astype(jnp.float32)
            for j in range(n_kv)
        ]
    )
    projected = projected.astype(jnp.bfloat16).astype(jnp.float32)

    low = low_ref[...]
    loads["state"].wait()
    for s in range(seqs):
        base = s * per_seq
        query_pre = projected[base : base + heads]
        forget_pre = projected[base + heads : base + 2 * heads]
        input_pre = projected[base + 2 * heads : base + 3 * heads]
        outgate_pre = projected[base + 3 * heads : base + 4 * heads]
        forget = low + (1.0 - low) * jax.nn.sigmoid(forget_pre)
        key_part = (1.0 - low) * jax.nn.sigmoid(-forget_pre)
        fill = jnp.zeros((HEAD - 3 * heads, HEAD), jnp.float32)
        turned = jnp.concatenate([forget, key_part, jax.nn.silu(query_pre), fill], axis=0).T
        readouts = []
        for h in range(heads):
            updated = (
                turned[:, h : h + 1] * state_v[s, h]
                + turned[:, heads + h : heads + h + 1] * input_pre[h : h + 1, :]
            )
            new_v[s, h] = updated
            query_col = turned[:, 2 * heads + h : 2 * heads + h + 1]
            readouts.append(jnp.sum(query_col * updated, axis=0, keepdims=True))
        readout = jnp.concatenate(readouts, axis=0)
        mean_square = jnp.mean(readout * readout, axis=1, keepdims=True)
        readout = readout * lax.rsqrt(mean_square + head_eps)
        gated_buf[s * heads : (s + 1) * heads, :] = (
            readout * head_gain_ref[...] * jax.nn.silu(outgate_pre)
        )
    store = pltpu.make_async_copy(new_v, state_out, store_sem)
    store.start()

    gated = jnp.concatenate(
        [gated_buf[pl.ds(h, seqs, stride=heads), :] for h in range(heads)], axis=1
    ).astype(jnp.bfloat16)
    loads["out"].wait()
    step = 4 * lane
    rows_tp = seqs * heads
    for k in range(0, width, step):
        part = jnp.dot(gated, out_v[:, k : k + step], preferred_element_type=jnp.float32)
        for j in range(step // lane):
            tile = k // lane + j
            first = (tile // heads) * rows_tp + tile % heads
            tp_f32[pl.ds(first, seqs, stride=heads), :] = part[:, j * lane : (j + 1) * lane]
    tp_send[...] = tp_f32[...].astype(jnp.bfloat16)

    def tp_peer(k):
        peer = lax.rem(tp + k, n_tp)
        return peer, (kv, peer)

    send_all(
        RS_TP, lambda i: slot(tp_send, i, rows_tp), slot(tp_recv, tp, rows_tp), n_tp, tp_peer
    )
    slot(tp_recv, tp, rows_tp)[...] = slot(tp_send, tp, rows_tp)[...]
    residual = jnp.concatenate(
        [
            normed_f32[pl.ds(tp * (heads * batch) + kv * seqs + s, heads, stride=batch), :]
            for s in range(seqs)
        ],
        axis=0,
    )
    wait_bytes(recv_sem.at[RS_TP], tp_recv, (n_tp - 1) * rows_tp)
    head_sum = tree_sum(
        [tp_recv[j * rows_tp : (j + 1) * rows_tp, :].astype(jnp.float32) for j in range(n_tp)]
    )
    stream_two = (residual_scale * residual + head_sum).astype(jnp.bfloat16)
    own_ag_two[...] = stream_two
    slot(ag_two, me, rows_tp)[...] = stream_two
    send_all(AG_TWO, lambda i: own_ag_two, slot(ag_two, me, rows_tp), n, peer_id)
    wait_bytes(recv_sem.at[AG_TWO], ag_two, (n - 1) * rows_tp)
    ag_two_f32[...] = ag_two[...].astype(jnp.float32)
    tiles = [
        jnp.concatenate(
            [
                ag_two_f32[
                    pl.ds((j // heads) * rows_tp + s * heads + j % heads, n_kv, stride=n_tp * rows_tp),
                    :,
                ]
                for s in range(seqs)
            ],
            axis=0,
        )
        for j in range(n)
    ]
    normed = [tile.astype(jnp.bfloat16) for tile in norm_tiles(tiles, 1)]
    wait_bytes(send_sem.at[RS_ONE], rs_recv_one, (n - 1) * batch)
    for j, tile in enumerate(normed):
        normed_bf[j * batch : (j + 1) * batch, :] = tile
    ffn(jnp.concatenate(normed, axis=1), 1)
    total = reduce_scatter(RS_THREE, rs_recv_three)
    residual = slot(normed_bf, me, batch)[...].astype(jnp.float32)
    stream = residual_scale * residual + 0.5 * total
    own_ag_three[...] = stream.astype(jnp.bfloat16)
    slot(ag_three, me, batch)[...] = stream.astype(jnp.bfloat16)
    send_all(AG_THREE, lambda i: own_ag_three, slot(ag_three, me, batch), n, peer_id)
    wait_bytes(recv_sem.at[AG_THREE], ag_three, (n - 1) * batch)
    mean, _, scale = stats(tiles_of(ag_three))
    mixed = (stream - mean) * scale * gb_own[2:3, :] + gb_own[5:6, :]
    for s in range(seqs):
        final_buf[pl.ds(s, n_kv, stride=seqs), :] = mixed[s * n_kv : (s + 1) * n_kv, :]
    mixed_ref[...] = final_buf[...].astype(jnp.bfloat16)

    for phase in (TOK, AG_ONE, AG_TWO, RS_THREE, AG_THREE):
        wait_bytes(send_sem.at[phase], tok_buf, (n - 1) * batch)
    wait_bytes(send_sem.at[GB], gb_buf, (n - 1) * 8)
    wait_bytes(send_sem.at[RS_KV], proj_recv, (n_kv - 1) * block_len)
    wait_bytes(send_sem.at[RS_TP], tp_recv, (n_tp - 1) * rows_tp)
    store.wait()


def fused(n_kv, n_tp, *args):
    (
        tokens,
        gate_weights,
        up_weights,
        down_weights,
        norm_gain,
        norm_bias,
        query_weight,
        forget_weight,
        input_weight,
        outgate_weight,
        lower_bound,
        head_gain,
        out_weight,
        state,
    ) = args
    batch, lane = tokens.shape
    n = n_kv * n_tp
    seqs, heads = state.shape[:2]
    gate_weights = jnp.swapaxes(gate_weights, 1, 2)
    up_weights = jnp.swapaxes(up_weights, 1, 2)
    bf16, f32 = jnp.bfloat16, jnp.float32
    per_seq = 4 * heads
    rows_tp = seqs * heads
    scratch = [
        pltpu.VMEM(gate_weights.shape, bf16),
        pltpu.VMEM(up_weights.shape, bf16),
        pltpu.VMEM(down_weights.shape, bf16),
        pltpu.VMEM((4, *query_weight.shape), bf16),
        pltpu.VMEM(out_weight.shape, bf16),
        pltpu.VMEM(state.shape, f32),
        pltpu.VMEM(state.shape, f32),
        pltpu.VMEM((n * batch, lane), bf16),
        pltpu.VMEM((8, lane), f32),
        pltpu.VMEM((n * 8, lane), f32),
        pltpu.VMEM((n * batch, lane), bf16),
        pltpu.VMEM((n * batch, lane), bf16),
        pltpu.VMEM((n * batch, lane), bf16),
        pltpu.VMEM((batch, lane), bf16),
        pltpu.VMEM((n * batch, lane), bf16),
        pltpu.VMEM((n * batch, lane), f32),
        pltpu.VMEM((n * batch, lane), bf16),
        pltpu.VMEM((batch * per_seq, HEAD), f32),
        pltpu.VMEM((batch * per_seq, HEAD), bf16),
        pltpu.VMEM((batch * per_seq, HEAD), bf16),
        pltpu.VMEM((rows_tp, HEAD), f32),
        pltpu.VMEM((n_tp * rows_tp, HEAD), f32),
        pltpu.VMEM((n_tp * rows_tp, HEAD), bf16),
        pltpu.VMEM((n_tp * rows_tp, HEAD), bf16),
        pltpu.VMEM((rows_tp, HEAD), bf16),
        pltpu.VMEM((n * rows_tp, HEAD), bf16),
        pltpu.VMEM((n * rows_tp, HEAD), f32),
        pltpu.VMEM((batch, lane), bf16),
        pltpu.VMEM((n * batch, lane), bf16),
        pltpu.VMEM((batch, lane), f32),
        pltpu.SemaphoreType.DMA((PHASES,)),
        pltpu.SemaphoreType.DMA((PHASES,)),
        pltpu.SemaphoreType.DMA((12,)),
        pltpu.SemaphoreType.DMA,
    ]
    vmem = pl.BlockSpec(memory_space=pltpu.VMEM)
    hbm = pl.BlockSpec(memory_space=pl.ANY)
    return pl.pallas_call(
        functools.partial(layer_kernel, n_kv, n_tp),
        out_shape=(
            jax.ShapeDtypeStruct(tokens.shape, bf16),
            jax.ShapeDtypeStruct(state.shape, f32),
        ),
        in_specs=[vmem] * 5 + [hbm] * 9,
        out_specs=(vmem, hbm),
        scratch_shapes=scratch,
        compiler_params=pltpu.CompilerParams(
            collective_id=0, has_side_effects=True, vmem_limit_bytes=60 * 1024 * 1024
        ),
        name="layer",
    )(
        tokens,
        norm_gain,
        norm_bias,
        lower_bound.reshape(heads, HEAD),
        head_gain.reshape(heads, HEAD),
        gate_weights,
        up_weights,
        down_weights,
        query_weight,
        forget_weight,
        input_weight,
        outgate_weight,
        out_weight,
        state,
    )


def dispatch(n_kv, n_tp, *args):
    tokens, state = args[0], args[13]
    batch, lane = tokens.shape
    whole_tiles = lane == HEAD and batch % 16 == 0 and (state.shape[0] * state.shape[1]) % 16 == 0
    if whole_tiles and state.shape[1] == 8 and n_kv % 8 == 0:
        return fused(n_kv, n_tp, *args)
    return local(*args)


def solution(mesh):
    n_kv, n_tp = mesh.shape["kv"], mesh.shape["tp"]
    return jax.shard_map(
        functools.partial(dispatch, n_kv, n_tp),
        mesh=mesh,
        in_specs=(
            P(None, ("kv", "tp")),
            P(None, None, ("kv", "tp")),
            P(None, None, ("kv", "tp")),
            P(None, ("kv", "tp"), None),
            P(None, ("kv", "tp")),
            P(None, ("kv", "tp")),
            P("kv", "tp"),
            P("kv", "tp"),
            P("kv", "tp"),
            P("kv", "tp"),
            P("tp"),
            P("tp"),
            P("tp", None),
            P("kv", "tp", None, None),
        ),
        out_specs=(P(None, ("kv", "tp")), P("kv", "tp", None, None)),
        check_vma=False,
    )
```

```python
import functools

import jax
import jax.numpy as jnp
from jax import lax
from jax.experimental import pallas as pl
from jax.experimental.pallas import tpu as pltpu
from jax.sharding import PartitionSpec as P

MESH = pl.DeviceIdType.MESH

HEAD = 128


residual_scale = 8.0**0.25
norm_eps = 1e-05
head_eps = 1e-06


def whole_norm(stream, gain_row, bias_row):
    row_mean = jnp.mean(stream, axis=-1, keepdims=True)
    centred = stream - row_mean
    spread = jnp.mean(centred * centred, axis=-1, keepdims=True)
    return centred * lax.rsqrt(spread + norm_eps) * gain_row.astype(jnp.float32) + bias_row.astype(
        jnp.float32
    )


def ffn_partial(whole_rows, gate_w, up_w, down_w):
    gate_proj = jnp.dot(whole_rows, gate_w, preferred_element_type=jnp.float32)
    up_proj = jnp.dot(whole_rows, up_w, preferred_element_type=jnp.float32)
    hidden = (jax.nn.silu(gate_proj) * up_proj).astype(jnp.bfloat16)
    return jnp.dot(hidden, down_w, preferred_element_type=jnp.float32)


def local(
    tokens,
    gate_weights,
    up_weights,
    down_weights,
    norm_gain,
    norm_bias,
    query_weight,
    forget_weight,
    input_weight,
    outgate_weight,
    lower_bound,
    head_gain,
    out_weight,
    state,
):
    own_cols = tokens.shape[1]
    col_offset = lax.axis_index(("kv", "tp")) * own_cols
    whole_tokens, whole_gain, whole_bias = (
        lax.all_gather(tokens, ("kv", "tp"), axis=1, tiled=True),
        lax.all_gather(norm_gain, ("kv", "tp"), axis=1, tiled=True),
        lax.all_gather(norm_bias, ("kv", "tp"), axis=1, tiled=True),
    )

    def finish(partial_value, residual_whole, index, want_whole):
        total = lax.psum(partial_value, ("kv", "tp"))
        stream = residual_scale * residual_whole + 0.5 * total
        normed = whole_norm(stream, whole_gain[index], whole_bias[index]).astype(jnp.bfloat16)
        if want_whole:
            return normed
        return lax.dynamic_slice_in_dim(normed, col_offset, own_cols, 1)

    partial_one = ffn_partial(whole_tokens, gate_weights[0], up_weights[0], down_weights[0])
    normed_one = finish(partial_one, whole_tokens.astype(jnp.float32), 0, True)
    seq_count = state.shape[0]
    head_count = state.shape[1]
    head_cols = query_weight.shape[1]
    weight_rows = query_weight.shape[0]
    seq_offset = lax.axis_index("kv") * seq_count
    block_rows = lax.dynamic_slice_in_dim(
        normed_one, lax.axis_index("kv") * weight_rows, weight_rows, 1
    )
    weights = (query_weight, forget_weight, input_weight, outgate_weight)
    projected = lax.psum_scatter(
        jnp.concatenate(
            [jnp.dot(block_rows, weight, preferred_element_type=jnp.float32) for weight in weights],
            axis=1,
        ).astype(jnp.bfloat16),
        "kv",
        scatter_dimension=0,
        tiled=True,
    )
    query_pre = projected[:, :head_cols].astype(jnp.float32).reshape(seq_count, head_count, HEAD)
    forget_pre = (
        projected[:, head_cols : 2 * head_cols]
        .astype(jnp.float32)
        .reshape(seq_count, head_count, HEAD)
    )
    input_pre = (
        projected[:, 2 * head_cols : 3 * head_cols]
        .astype(jnp.float32)
        .reshape(seq_count, head_count, HEAD)
    )
    outgate_pre = projected[:, 3 * head_cols :].astype(jnp.float32)
    low_bound = lower_bound.reshape(head_count, HEAD)
    forget = low_bound + (1.0 - low_bound) * jax.nn.sigmoid(forget_pre)
    key_part = (1.0 - low_bound) * jax.nn.sigmoid(-forget_pre)
    updated = forget[..., None] * state + key_part[..., None] * input_pre[:, :, None, :]
    readout = jnp.einsum(
        "shd,shde->she", jax.nn.silu(query_pre), updated, precision=lax.Precision.HIGHEST
    )
    readout = readout * lax.rsqrt(jnp.mean(readout * readout, axis=-1, keepdims=True) + head_eps)
    gated_out = (
        readout.reshape(seq_count, head_cols) * head_gain * jax.nn.silu(outgate_pre)
    ).astype(jnp.bfloat16)
    mixer_part = jnp.dot(gated_out, out_weight, preferred_element_type=jnp.float32)
    head_sum = lax.psum_scatter(
        mixer_part.astype(jnp.bfloat16), "tp", scatter_dimension=1, tiled=True
    ).astype(jnp.float32)
    piece_cols = head_sum.shape[1]
    own_normed = lax.dynamic_slice_in_dim(normed_one, seq_offset, seq_count, 0)
    own_normed = lax.dynamic_slice_in_dim(
        own_normed, lax.axis_index("tp") * piece_cols, piece_cols, 1
    )
    stream_own = (residual_scale * own_normed.astype(jnp.float32) + head_sum).astype(jnp.bfloat16)
    seq_rows = lax.all_gather(stream_own, "tp", axis=1, tiled=True)
    stream_two = lax.all_gather(seq_rows, "kv", axis=0, tiled=True)
    normed_two = whole_norm(stream_two.astype(jnp.float32), whole_gain[1], whole_bias[1]).astype(
        jnp.bfloat16
    )
    partial_two = ffn_partial(normed_two, gate_weights[1], up_weights[1], down_weights[1])
    mixed = finish(partial_two, normed_two.astype(jnp.float32), 2, False)
    return (mixed, updated)


TOK, GB, RS_ONE, AG_ONE, RS_KV, RS_TP, AG_TWO, RS_THREE, AG_THREE = range(9)
PHASES = 9


def tree_sum(terms):
    while len(terms) > 1:
        rest = [terms[-1]] if len(terms) % 2 else []
        terms = [a + b for a, b in zip(terms[::2], terms[1::2])] + rest
    return terms[0]


def dot_turned(rows, weights):
    return lax.dot_general(
        rows, weights, (((1,), (1,)), ((), ())), preferred_element_type=jnp.float32
    )


def layer_kernel(
    n_kv,
    n_tp,
    tokens_ref,
    gain_ref,
    bias_ref,
    low_ref,
    head_gain_ref,
    gate_hbm,
    up_hbm,
    down_hbm,
    query_hbm,
    forget_hbm,
    input_hbm,
    outgate_hbm,
    out_hbm,
    state_hbm,
    mixed_ref,
    state_out,
    gate_v,
    up_v,
    down_v,
    proj_v,
    out_v,
    state_v,
    new_v,
    tok_buf,
    gb_own,
    gb_buf,
    rs_send,
    rs_recv_one,
    rs_recv_three,
    own_ag,
    ag_one,
    normed_f32,
    normed_bf,
    proj_f32,
    proj_send,
    proj_recv,
    gated_buf,
    tp_f32,
    tp_send,
    tp_recv,
    own_ag_two,
    ag_two,
    ag_two_f32,
    own_ag_three,
    ag_three,
    final_buf,
    send_sem,
    recv_sem,
    load_sem,
    store_sem,
):
    n = n_kv * n_tp
    batch, lane = tokens_ref.shape
    width = n * lane
    seqs, heads = state_v.shape[0], state_v.shape[1]
    kv, tp = lax.axis_index("kv"), lax.axis_index("tp")
    me = kv * n_tp + tp

    proj_hbm = (query_hbm, forget_hbm, input_hbm, outgate_hbm)
    loads = {}
    order = [("gate0", gate_hbm.at[0], gate_v.at[0]), ("up0", up_hbm.at[0], up_v.at[0])]
    order += [("down0", down_hbm.at[0], down_v.at[0])]
    order += [("proj%d" % i, proj_hbm[i], proj_v.at[i]) for i in range(4)]
    order += [("state", state_hbm, state_v), ("out", out_hbm, out_v)]
    order += [("gate1", gate_hbm.at[1], gate_v.at[1]), ("up1", up_hbm.at[1], up_v.at[1])]
    order += [("down1", down_hbm.at[1], down_v.at[1])]
    for i, (name, source, target) in enumerate(order):
        loads[name] = pltpu.make_async_copy(source, target, load_sem.at[i])
        loads[name].start()

    def turn(index, by, count):
        moved = index + by
        return jnp.where(moved >= count, moved - count, moved)

    def peer_id(k):
        far, near = divmod(k, n_tp)
        peer = (turn(kv, far, n_kv), turn(tp, near, n_tp))
        return peer[0] * n_tp + peer[1], peer

    barrier = pltpu.get_barrier_semaphore()

    for k in range(1, n):
        _, device = peer_id(k)
        pl.semaphore_signal(barrier, inc=1, device_id=device, device_id_type=MESH)

    def slot(ref, index, rows):
        return ref.at[pl.ds(pl.multiple_of(index * rows, rows), rows)]

    def send_all(phase, src_of, dst, count, device_of):
        for k in sorted(range(1, count), key=lambda k: abs(2 * k - count)):
            index, device = device_of(k)
            pltpu.make_async_remote_copy(
                src_ref=src_of(index),
                dst_ref=dst,
                send_sem=send_sem.at[phase],
                recv_sem=recv_sem.at[phase],
                device_id=device,
                device_id_type=MESH,
            ).start()

    def wait_bytes(sem, ref, rows):
        part = ref.at[pl.ds(0, rows)]
        pltpu.make_async_copy(part, part, sem).wait()

    gb_own[...] = jnp.zeros(gb_own.shape, jnp.float32)
    gb_own[0:3, :] = gain_ref[...].astype(jnp.float32)
    gb_own[3:6, :] = bias_ref[...].astype(jnp.float32)
    slot(gb_buf, me, 8)[...] = gb_own[...]
    slot(tok_buf, me, batch)[...] = tokens_ref[...]

    pl.semaphore_wait(barrier, n - 1)
    send_all(TOK, lambda i: tokens_ref, slot(tok_buf, me, batch), n, peer_id)
    send_all(GB, lambda i: gb_own, slot(gb_buf, me, 8), n, peer_id)

    def tiles_of(ref):
        return [ref[j * batch : (j + 1) * batch, :].astype(jnp.float32) for j in range(n)]

    def stats(tiles):
        mean = jnp.sum(tree_sum(tiles), axis=1, keepdims=True) / width
        centred = [tile - mean for tile in tiles]
        spread = jnp.sum(tree_sum([c * c for c in centred]), axis=1, keepdims=True) / width
        return mean, centred, lax.rsqrt(spread + norm_eps)

    def norm_tiles(tiles, index):
        _, centred, scale = stats(tiles)
        return [
            c * scale * gb_buf[8 * j + index : 8 * j + index + 1, :]
            + gb_buf[8 * j + 3 + index : 8 * j + 4 + index, :]
            for j, c in enumerate(centred)
        ]

    def ffn(rows, layer):
        step = 4 * lane
        gate = jnp.zeros((batch, gate_v.shape[1]), jnp.float32)
        up = jnp.zeros((batch, gate_v.shape[1]), jnp.float32)
        loads["gate%d" % layer].wait()
        loads["up%d" % layer].wait()
        for k in range(0, width, step):
            piece = rows[:, k : k + step]
            gate += dot_turned(piece, gate_v[layer, :, k : k + step])
            up += dot_turned(piece, up_v[layer, :, k : k + step])
        hidden = (jax.nn.silu(gate) * up).astype(jnp.bfloat16)
        loads["down%d" % layer].wait()
        for k in range(0, width, step):
            part = jnp.dot(
                hidden, down_v[layer, :, k : k + step], preferred_element_type=jnp.float32
            ).astype(jnp.bfloat16)
            for j in range(step // lane):
                first = (k // lane + j) * batch
                rs_send[first : first + batch, :] = part[:, j * lane : (j + 1) * lane]

    def reduce_scatter(phase, recv):
        send_all(phase, lambda i: slot(rs_send, i, batch), slot(recv, me, batch), n, peer_id)
        slot(recv, me, batch)[...] = slot(rs_send, me, batch)[...]
        wait_bytes(recv_sem.at[phase], recv, (n - 1) * batch)
        return tree_sum(tiles_of(recv))

    wait_bytes(recv_sem.at[TOK], tok_buf, (n - 1) * batch)
    ffn(jnp.concatenate([tok_buf[j * batch : (j + 1) * batch, :] for j in range(n)], axis=1), 0)
    total = reduce_scatter(RS_ONE, rs_recv_one)
    stream = residual_scale * tokens_ref[...].astype(jnp.float32) + 0.5 * total
    own_ag[...] = stream.astype(jnp.bfloat16)
    slot(ag_one, me, batch)[...] = stream.astype(jnp.bfloat16)
    send_all(AG_ONE, lambda i: own_ag, slot(ag_one, me, batch), n, peer_id)
    wait_bytes(recv_sem.at[GB], gb_buf, (n - 1) * 8)
    wait_bytes(recv_sem.at[AG_ONE], ag_one, (n - 1) * batch)
    for j, tile in enumerate(norm_tiles(tiles_of(ag_one), 0)):
        rounded = tile.astype(jnp.bfloat16)
        normed_bf[j * batch : (j + 1) * batch, :] = rounded
        normed_f32[j * batch : (j + 1) * batch, :] = rounded.astype(jnp.float32)

    own_rows = slot(normed_bf, kv, n_tp * batch)
    block = jnp.concatenate(
        [own_rows[j * batch : (j + 1) * batch, :] for j in range(n_tp)], axis=1
    )
    per_seq = 4 * heads
    for i in range(4):
        loads["proj%d" % i].wait()
        part = jnp.dot(block, proj_v[i], preferred_element_type=jnp.float32)
        for h in range(heads):
            for r in range(0, batch, 8):
                proj_f32[pl.ds(r * per_seq + i * heads + h, 8, stride=per_seq), :] = part[
                    r : r + 8, h * HEAD : (h + 1) * HEAD
                ]
    proj_send[...] = proj_f32[...].astype(jnp.bfloat16)
    block_len = seqs * per_seq

    def kv_peer(k):
        peer = turn(kv, k, n_kv)
        return peer, (peer, tp)

    send_all(
        RS_KV,
        lambda i: slot(proj_send, i, block_len),
        slot(proj_recv, kv, block_len),
        n_kv,
        kv_peer,
    )
    slot(proj_recv, kv, block_len)[...] = slot(proj_send, kv, block_len)[...]
    wait_bytes(recv_sem.at[RS_KV], proj_recv, (n_kv - 1) * block_len)
    projected = tree_sum(
        [
            proj_recv[j * block_len : (j + 1) * block_len, :].astype(jnp.float32)
            for j in range(n_kv)
        ]
    )
    projected = projected.astype(jnp.bfloat16).astype(jnp.float32)

    low = low_ref[...]
    loads["state"].wait()
    for s in range(seqs):
        base = s * per_seq
        query_pre = projected[base : base + heads]
        forget_pre = projected[base + heads : base + 2 * heads]
        input_pre = projected[base + 2 * heads : base + 3 * heads]
        outgate_pre = projected[base + 3 * heads : base + 4 * heads]
        forget = low + (1.0 - low) * jax.nn.sigmoid(forget_pre)
        key_part = (1.0 - low) * jax.nn.sigmoid(-forget_pre)
        fill = jnp.zeros((HEAD - 3 * heads, HEAD), jnp.float32)
        turned = jnp.concatenate([forget, key_part, jax.nn.silu(query_pre), fill], axis=0).T
        readouts = []
        for h in range(heads):
            updated = (
                turned[:, h : h + 1] * state_v[s, h]
                + turned[:, heads + h : heads + h + 1] * input_pre[h : h + 1, :]
            )
            new_v[s, h] = updated
            query_col = turned[:, 2 * heads + h : 2 * heads + h + 1]
            readouts.append(jnp.sum(query_col * updated, axis=0, keepdims=True))
        readout = jnp.concatenate(readouts, axis=0)
        mean_square = jnp.mean(readout * readout, axis=1, keepdims=True)
        readout = readout * lax.rsqrt(mean_square + head_eps)
        gated_buf[s * heads : (s + 1) * heads, :] = (
            readout * head_gain_ref[...] * jax.nn.silu(outgate_pre)
        )
    store = pltpu.make_async_copy(new_v, state_out, store_sem)
    store.start()

    gated = jnp.concatenate(
        [gated_buf[pl.ds(h, seqs, stride=heads), :] for h in range(heads)], axis=1
    ).astype(jnp.bfloat16)
    loads["out"].wait()
    step = 4 * lane
    rows_tp = seqs * heads
    for k in range(0, width, step):
        part = jnp.dot(gated, out_v[:, k : k + step], preferred_element_type=jnp.float32)
        for j in range(step // lane):
            tile = k // lane + j
            first = (tile // heads) * rows_tp + tile % heads
            tp_f32[pl.ds(first, seqs, stride=heads), :] = part[:, j * lane : (j + 1) * lane]
    tp_send[...] = tp_f32[...].astype(jnp.bfloat16)

    def tp_peer(k):
        peer = turn(tp, k, n_tp)
        return peer, (kv, peer)

    send_all(
        RS_TP, lambda i: slot(tp_send, i, rows_tp), slot(tp_recv, tp, rows_tp), n_tp, tp_peer
    )
    slot(tp_recv, tp, rows_tp)[...] = slot(tp_send, tp, rows_tp)[...]
    residual = jnp.concatenate(
        [
            normed_f32[pl.ds(tp * (heads * batch) + kv * seqs + s, heads, stride=batch), :]
            for s in range(seqs)
        ],
        axis=0,
    )
    wait_bytes(recv_sem.at[RS_TP], tp_recv, (n_tp - 1) * rows_tp)
    head_sum = tree_sum(
        [tp_recv[j * rows_tp : (j + 1) * rows_tp, :].astype(jnp.float32) for j in range(n_tp)]
    )
    stream_two = (residual_scale * residual + head_sum).astype(jnp.bfloat16)
    own_ag_two[...] = stream_two
    slot(ag_two, me, rows_tp)[...] = stream_two
    send_all(AG_TWO, lambda i: own_ag_two, slot(ag_two, me, rows_tp), n, peer_id)
    wait_bytes(recv_sem.at[AG_TWO], ag_two, (n - 1) * rows_tp)
    ag_two_f32[...] = ag_two[...].astype(jnp.float32)
    tiles = [
        jnp.concatenate(
            [
                ag_two_f32[
                    pl.ds((j // heads) * rows_tp + s * heads + j % heads, n_kv, stride=n_tp * rows_tp),
                    :,
                ]
                for s in range(seqs)
            ],
            axis=0,
        )
        for j in range(n)
    ]
    normed = [tile.astype(jnp.bfloat16) for tile in norm_tiles(tiles, 1)]
    wait_bytes(send_sem.at[RS_ONE], rs_recv_one, (n - 1) * batch)
    for j, tile in enumerate(normed):
        normed_bf[j * batch : (j + 1) * batch, :] = tile
    ffn(jnp.concatenate(normed, axis=1), 1)
    total = reduce_scatter(RS_THREE, rs_recv_three)
    residual = slot(normed_bf, me, batch)[...].astype(jnp.float32)
    stream = residual_scale * residual + 0.5 * total
    own_ag_three[...] = stream.astype(jnp.bfloat16)
    slot(ag_three, me, batch)[...] = stream.astype(jnp.bfloat16)
    send_all(AG_THREE, lambda i: own_ag_three, slot(ag_three, me, batch), n, peer_id)
    wait_bytes(recv_sem.at[AG_THREE], ag_three, (n - 1) * batch)
    mean, _, scale = stats(tiles_of(ag_three))
    mixed = (stream - mean) * scale * gb_own[2:3, :] + gb_own[5:6, :]
    for s in range(seqs):
        final_buf[pl.ds(s, n_kv, stride=seqs), :] = mixed[s * n_kv : (s + 1) * n_kv, :]
    mixed_ref[...] = final_buf[...].astype(jnp.bfloat16)

    for phase in (TOK, AG_ONE, AG_TWO, RS_THREE, AG_THREE):
        wait_bytes(send_sem.at[phase], tok_buf, (n - 1) * batch)
    wait_bytes(send_sem.at[GB], gb_buf, (n - 1) * 8)
    wait_bytes(send_sem.at[RS_KV], proj_recv, (n_kv - 1) * block_len)
    wait_bytes(send_sem.at[RS_TP], tp_recv, (n_tp - 1) * rows_tp)
    store.wait()


def fused(n_kv, n_tp, *args):
    (
        tokens,
        gate_weights,
        up_weights,
        down_weights,
        norm_gain,
        norm_bias,
        query_weight,
        forget_weight,
        input_weight,
        outgate_weight,
        lower_bound,
        head_gain,
        out_weight,
        state,
    ) = args
    batch, lane = tokens.shape
    n = n_kv * n_tp
    seqs, heads = state.shape[:2]
    gate_weights = jnp.swapaxes(gate_weights, 1, 2)
    up_weights = jnp.swapaxes(up_weights, 1, 2)
    bf16, f32 = jnp.bfloat16, jnp.float32
    per_seq = 4 * heads
    rows_tp = seqs * heads
    scratch = [
        pltpu.VMEM(gate_weights.shape, bf16),
        pltpu.VMEM(up_weights.shape, bf16),
        pltpu.VMEM(down_weights.shape, bf16),
        pltpu.VMEM((4, *query_weight.shape), bf16),
        pltpu.VMEM(out_weight.shape, bf16),
        pltpu.VMEM(state.shape, f32),
        pltpu.VMEM(state.shape, f32),
        pltpu.VMEM((n * batch, lane), bf16),
        pltpu.VMEM((8, lane), f32),
        pltpu.VMEM((n * 8, lane), f32),
        pltpu.VMEM((n * batch, lane), bf16),
        pltpu.VMEM((n * batch, lane), bf16),
        pltpu.VMEM((n * batch, lane), bf16),
        pltpu.VMEM((batch, lane), bf16),
        pltpu.VMEM((n * batch, lane), bf16),
        pltpu.VMEM((n * batch, lane), f32),
        pltpu.VMEM((n * batch, lane), bf16),
        pltpu.VMEM((batch * per_seq, HEAD), f32),
        pltpu.VMEM((batch * per_seq, HEAD), bf16),
        pltpu.VMEM((batch * per_seq, HEAD), bf16),
        pltpu.VMEM((rows_tp, HEAD), f32),
        pltpu.VMEM((n_tp * rows_tp, HEAD), f32),
        pltpu.VMEM((n_tp * rows_tp, HEAD), bf16),
        pltpu.VMEM((n_tp * rows_tp, HEAD), bf16),
        pltpu.VMEM((rows_tp, HEAD), bf16),
        pltpu.VMEM((n * rows_tp, HEAD), bf16),
        pltpu.VMEM((n * rows_tp, HEAD), f32),
        pltpu.VMEM((batch, lane), bf16),
        pltpu.VMEM((n * batch, lane), bf16),
        pltpu.VMEM((batch, lane), f32),
        pltpu.SemaphoreType.DMA((PHASES,)),
        pltpu.SemaphoreType.DMA((PHASES,)),
        pltpu.SemaphoreType.DMA((12,)),
        pltpu.SemaphoreType.DMA,
    ]
    vmem = pl.BlockSpec(memory_space=pltpu.VMEM)
    hbm = pl.BlockSpec(memory_space=pl.ANY)
    return pl.pallas_call(
        functools.partial(layer_kernel, n_kv, n_tp),
        out_shape=(
            jax.ShapeDtypeStruct(tokens.shape, bf16),
            jax.ShapeDtypeStruct(state.shape, f32),
        ),
        in_specs=[vmem] * 5 + [hbm] * 9,
        out_specs=(vmem, hbm),
        scratch_shapes=scratch,
        compiler_params=pltpu.CompilerParams(
            collective_id=0, has_side_effects=True, vmem_limit_bytes=60 * 1024 * 1024
        ),
        name="layer",
    )(
        tokens,
        norm_gain,
        norm_bias,
        lower_bound.reshape(heads, HEAD),
        head_gain.reshape(heads, HEAD),
        gate_weights,
        up_weights,
        down_weights,
        query_weight,
        forget_weight,
        input_weight,
        outgate_weight,
        out_weight,
        state,
    )


def dispatch(n_kv, n_tp, *args):
    tokens, state = args[0], args[13]
    batch, lane = tokens.shape
    whole_tiles = lane == HEAD and batch % 16 == 0 and (state.shape[0] * state.shape[1]) % 16 == 0
    if whole_tiles and state.shape[1] == 8 and n_kv % 8 == 0:
        return fused(n_kv, n_tp, *args)
    return local(*args)


def solution(mesh):
    n_kv, n_tp = mesh.shape["kv"], mesh.shape["tp"]
    return jax.shard_map(
        functools.partial(dispatch, n_kv, n_tp),
        mesh=mesh,
        in_specs=(
            P(None, ("kv", "tp")),
            P(None, None, ("kv", "tp")),
            P(None, None, ("kv", "tp")),
            P(None, ("kv", "tp"), None),
            P(None, ("kv", "tp")),
            P(None, ("kv", "tp")),
            P("kv", "tp"),
            P("kv", "tp"),
            P("kv", "tp"),
            P("kv", "tp"),
            P("tp"),
            P("tp"),
            P("tp", None),
            P("kv", "tp", None, None),
        ),
        out_specs=(P(None, ("kv", "tp")), P("kv", "tp", None, None)),
        check_vma=False,
    )
```
